32 devices in a mesh: sp: 16 (over z, y, x), tp: 2 (over core).
Axes of the slice: x: 2, y: 2, z: 4, core: 2. Of those that a mesh axis runs over, the one named last changes fastest.
Arguments:
- query_one: bfloat16 [2048, 1024], P('sp', 'tp'), may hold values from -6 to 6
- key_one: bfloat16 [2048, 1024], P('sp', 'tp'), may hold values from -6 to 6
- query_two: bfloat16 [2048, 512], P('sp', 'tp'), may hold values from -6 to 6
- key_two: bfloat16 [2048, 512], P('sp', 'tp'), may hold values from -6 to 6
- values: bfloat16 [2048, 2048], P('sp', 'tp'), may hold values from -6 to 6
- out_gate: bfloat16 [2048, 2048], P('sp', 'tp'), may hold values from -6 to 6
- in_gate: float32 [16, 2048], P('tp', 'sp'), may hold values from -3 to 150
- forget_gate: float32 [16, 2048], P('tp', 'sp'), may hold values from -1 to 24
- head_gain: float32 [2048], P('tp'), may hold values from 0.1 to 1.9
- out_weight: bfloat16 [2048, 2048], P('tp'), may hold values from -0.125 to 0.125
- stream: bfloat16 [2048, 2048], P('sp'), may hold values from -6 to 6
- mix_gain: float32 [2048], replicated, may hold values from 0.1 to 1.9
- up_weight: bfloat16 [2048, 8192], P('sp', 'tp'), may hold values from -0.125 to 0.125
- down_weight: bfloat16 [8192, 2048], P('tp', 'sp'), may hold values from -0.0625 to 0.0625
- out_gain: float32 [2048], replicated, may hold values from 0.1 to 1.9
Outputs:
- result: bfloat16 [2048, 2048], P(('sp', 'tp'))
The draws below stay inside these ranges and needn't reach their ends.
All inputs are finite; a program needn't handle non-finite values.
Results may differ from the reference program's by a relative error of at most 0.018.
Values may be sent and summed in bfloat16 or wider, within the bound.
A program may use at most 128 MiB of HBM per device.

```python
import jax
import jax.numpy as jnp
from jax import lax

D = 2048
HEADS = 8
KA = 128
KB = 64
DV = 128
FF = 8192
BLOCK = 64
TOK_DEV = 128
SEQUENCE_TOKENS = 2048
MIX = 2048
GATE_HEADS = 16
N_TP = 2


def draw_forget_gate(key, part):
    merged_keys = jax.random.split(jax.random.fold_in(key, 11), 5)
    slow_share = 0.5
    noise = jnp.clip(jax.random.normal(merged_keys[1], (GATE_HEADS, SEQUENCE_TOKENS), jnp.float32), -3.0, 3.0)
    slow_heads = jax.random.uniform(merged_keys[0], (GATE_HEADS, 1), jnp.float32) < slow_share
    base_level = jnp.where(slow_heads, jnp.log(SEQUENCE_TOKENS / 0.3), jnp.log(40.0))
    device_shift = jax.random.uniform(merged_keys[2], (1, SEQUENCE_TOKENS // TOK_DEV), jnp.float32, -0.7, 0.7)
    device_shift = jnp.repeat(device_shift, TOK_DEV, axis=1)
    level_values = base_level + noise + device_shift
    spike_locations = jax.random.randint(merged_keys[3], (GATE_HEADS, 3), 0, SEQUENCE_TOKENS)
    token_positions = jnp.arange(SEQUENCE_TOKENS, dtype=jnp.int32)
    spike_mask = jnp.any(token_positions[None, None, :] == spike_locations[:, :, None], 1)
    spike_level = jax.random.uniform(merged_keys[4], (GATE_HEADS, SEQUENCE_TOKENS), jnp.float32, 0.3, 1.4)
    return jnp.where(spike_mask, spike_level, level_values).astype(jnp.float32)


def draw_in_gate(key, part):
    merged_keys = jax.random.split(jax.random.fold_in(key, 23), 1)
    level_values = jnp.clip(jax.random.normal(merged_keys[0], (GATE_HEADS, SEQUENCE_TOKENS), jnp.float32), -3.0, 3.0)
    return level_values.astype(jnp.float32)


def level_of(stream_key, shape, cuts, smallest, largest):
    level, own = 1.0, jax.random.fold_in(stream_key, 6)
    for dim, parts in cuts:
        steps = jnp.exp(jax.random.uniform(jax.random.fold_in(own, dim), (parts,), jnp.float32, smallest / len(cuts), largest / len(cuts)))
        level = level * jnp.repeat(steps, shape[dim] // parts).reshape([-1 if axis == dim else 1 for axis in range(len(shape))])
    return level


def gaussian(own_key, extent, deviation, bound, cuts=(), kind=jnp.bfloat16):
    drawn = jax.random.normal(own_key, extent, jnp.float32) * deviation
    if len(cuts) > 0:
        drawn = level_of(own_key, extent, cuts, -0.22, 0.18) * drawn
    return jnp.clip(drawn, min=-bound, max=bound).astype(kind)


def setup_inputs(seed: int = 0) -> dict:
    splits = jax.random.split(jax.random.key(seed), 16)
    query_one = gaussian(splits[0], (SEQUENCE_TOKENS, HEADS * KA), 1.0, 6.0, ((0, 16), (1, 2)))
    key_one = gaussian(splits[1], (SEQUENCE_TOKENS, HEADS * KA), 1.0, 6.0, ((0, 16), (1, 2)))
    query_two = gaussian(splits[2], (SEQUENCE_TOKENS, HEADS * KB), 1.0, 6.0, ((0, 16), (1, 2)))
    key_two = gaussian(splits[3], (SEQUENCE_TOKENS, HEADS * KB), 1.0, 6.0, ((0, 16), (1, 2)))
    values = gaussian(splits[4], (SEQUENCE_TOKENS, MIX), 1.0, 6.0, ((0, 16), (1, 2)))
    out_gate = gaussian(splits[5], (SEQUENCE_TOKENS, MIX), 1.5, 6.0, ((0, 16), (1, 2)))
    in_gate = draw_in_gate(jax.random.fold_in(splits[15], 71), 0)
    forget_gate = draw_forget_gate(jax.random.fold_in(splits[15], 71), 0)
    head_gain = jnp.clip(1.0 + 0.18 * jax.random.normal(splits[8], (MIX,), jnp.float32), 0.1, 1.9)
    out_weight = gaussian(splits[9], (MIX, D), MIX ** -0.5, 0.125, ((0, 2),))
    stream = gaussian(splits[10], (SEQUENCE_TOKENS, D), 1.0, 6.0, ((0, 16),))
    mix_gain = jnp.clip(1.0 + 0.18 * jax.random.normal(splits[11], (D,), jnp.float32), 0.1, 1.9)
    up_weight = gaussian(splits[12], (D, FF), D ** -0.5, 0.125, ((0, 16), (1, 2)))
    down_weight = gaussian(splits[13], (FF, D), FF ** -0.5, 0.0625, ((0, 2), (1, 16)))
    out_gain = jnp.clip(1.0 + 0.18 * jax.random.normal(splits[14], (D,), jnp.float32), 0.1, 1.9)
    return dict(query_one=query_one, key_one=key_one, query_two=query_two, key_two=key_two, values=values, out_gate=out_gate, in_gate=in_gate, forget_gate=forget_gate, head_gain=head_gain, out_weight=out_weight, stream=stream, mix_gain=mix_gain, up_weight=up_weight, down_weight=down_weight, out_gain=out_gain)


NEG_BIG = -1e+30
EPS = 1e-05

def combine(earlier, later):
    decay_early, cell_early, norm_early, peak_early = earlier
    decay_late, cell_late, norm_late, peak_late = later
    ceiling = jnp.maximum(decay_late + peak_early, peak_late)
    keep_share = jnp.exp(decay_late + peak_early - ceiling)
    fresh_share = jnp.exp(peak_late - ceiling)
    cell_new = keep_share[..., None, None] * cell_early + fresh_share[..., None, None] * cell_late
    norm_new = keep_share[..., None] * norm_early + fresh_share[..., None] * norm_late
    return (decay_early + decay_late, cell_new, norm_new, ceiling)

def summarize(queries, keys_in, values_in, in_pre, forget_pre, block_len):
    length, width_k = queries.shape
    block_count = length // block_len
    scaled_keys = keys_in.astype(jnp.float32).reshape(block_count, block_len, width_k) * width_k ** (-0.5)
    values_f = values_in.astype(jnp.float32).reshape(block_count, block_len, -1)
    width_v = values_f.shape[-1]
    log_forget = jax.nn.log_sigmoid(forget_pre).reshape(block_count, block_len)
    log_input = in_pre.reshape(block_count, block_len)
    cumulative = jnp.cumsum(log_forget, 1)
    decay_total = cumulative[:, -1]
    weight_log = decay_total[:, None] - cumulative + log_input
    peak_log = lax.optimization_barrier(jnp.max(weight_log, 1))
    weighted = jnp.exp(weight_log - peak_log[:, None])[..., None] * scaled_keys
    cell_states = jnp.einsum('cld,cle->cde', weighted, values_f, precision=lax.Precision.HIGHEST)
    norm_states = lax.optimization_barrier(jnp.sum(weighted, 1))
    identity = (jnp.zeros((), jnp.float32), jnp.zeros((width_k, width_v), jnp.float32), jnp.zeros((width_k,), jnp.float32), jnp.full((), NEG_BIG, jnp.float32))

    def advance(running, element):
        return (combine(running, element), running)
    closing, prefix = lax.scan(advance, identity, (decay_total, cell_states, norm_states, peak_log))
    return (closing, prefix, (scaled_keys, values_f, cumulative, log_input))

def finish(queries, prefix, pieces, incoming):
    scaled_keys, values_f, cumulative, log_input = pieces
    block_count, block_len, width_k = scaled_keys.shape
    spread_in = jax.tree.map(lambda leaf: jnp.broadcast_to(leaf, (block_count,) + leaf.shape), incoming)
    _, cell_states, norm_states, peaks = combine(spread_in, prefix)
    query_f = queries.astype(jnp.float32).reshape(block_count, block_len, width_k)
    log_gaps = cumulative[:, :, None] - cumulative[:, None, :] + log_input[:, None, :]
    causal = jnp.arange(block_len)[:, None] >= jnp.arange(block_len)[None, :]
    log_gaps = jnp.where(causal[None], log_gaps, -jnp.inf)
    carried = cumulative + peaks[:, None]
    ceiling = jnp.maximum(carried, lax.optimization_barrier(jnp.max(log_gaps, 2)))
    scores = jnp.einsum('cld,csd->cls', query_f, scaled_keys, precision=lax.Precision.HIGHEST)
    scores = scores * jnp.exp(log_gaps - ceiling[..., None])
    carry_weight = jnp.exp(carried - ceiling)
    numerator = carry_weight[..., None] * jnp.einsum('cld,cde->cle', query_f, cell_states, precision=lax.Precision.HIGHEST)
    numerator = numerator + jnp.einsum('cls,cse->cle', scores, values_f, precision=lax.Precision.HIGHEST)
    denominator = carry_weight * jnp.einsum('cld,cd->cl', query_f, norm_states, precision=lax.Precision.HIGHEST)
    denominator = denominator + lax.optimization_barrier(jnp.sum(scores, 2))
    result = numerator / jnp.maximum(jnp.abs(denominator), jnp.exp(-ceiling))[..., None]
    return result.reshape(block_count * block_len, -1)

def run_head(queries, keys_in, values_in, in_pre, forget_pre):
    closing, prefix, pieces = summarize(queries, keys_in, values_in, in_pre, forget_pre, BLOCK)
    identity = jax.tree.map(lambda leaf: jnp.zeros_like(leaf), closing)
    identity = (identity[0], identity[1], identity[2], jnp.full((), NEG_BIG, jnp.float32))
    return finish(queries, prefix, pieces, identity)

def head_norm(cell_out):
    center = lax.optimization_barrier(jnp.mean(cell_out, -1, keepdims=True))
    spread = lax.optimization_barrier(jnp.mean(jnp.square(cell_out - center), -1, keepdims=True))
    return (cell_out - center) * lax.rsqrt(spread + EPS)

def layer_norm(rows_f, gain):
    center = lax.optimization_barrier(jnp.mean(rows_f, -1, keepdims=True))
    spread = lax.optimization_barrier(jnp.mean(jnp.square(rows_f - center), -1, keepdims=True))
    return (rows_f - center) * lax.rsqrt(spread + EPS) * gain

def reference(query_one, key_one, query_two, key_two, values, out_gate, in_gate, forget_gate, head_gain, out_weight, stream, mix_gain, up_weight, down_weight, out_gain):
    columns = []
    for pair_index in range(HEADS):
        base_v = 2 * pair_index * DV
        out_one = run_head(query_one[:, pair_index * KA:(pair_index + 1) * KA], key_one[:, pair_index * KA:(pair_index + 1) * KA], values[:, base_v:base_v + DV], in_gate[2 * pair_index], forget_gate[2 * pair_index])
        out_two = run_head(query_two[:, pair_index * KB:(pair_index + 1) * KB], key_two[:, pair_index * KB:(pair_index + 1) * KB], values[:, base_v + DV:base_v + 2 * DV], in_gate[2 * pair_index + 1], forget_gate[2 * pair_index + 1])
        columns.append(head_norm(out_one))
        columns.append(head_norm(out_two))
    normed = jnp.concatenate(columns, 1)
    mixed_heads = (normed * head_gain * jax.nn.sigmoid(out_gate.astype(jnp.float32))).astype(jnp.bfloat16)
    group_width = MIX // N_TP
    summed = jnp.zeros((SEQUENCE_TOKENS, D), jnp.float32)
    for group in range(N_TP):
        partial_sum = jnp.dot(mixed_heads[:, group * group_width:(group + 1) * group_width], out_weight[group * group_width:(group + 1) * group_width], preferred_element_type=jnp.float32).astype(jnp.bfloat16)
        summed = summed + lax.optimization_barrier(partial_sum).astype(jnp.float32)
    mixer_out = lax.optimization_barrier(summed.astype(jnp.bfloat16))
    first_norm = layer_norm(stream.astype(jnp.float32) + mixer_out.astype(jnp.float32), mix_gain).astype(jnp.bfloat16)
    hidden_width = FF // N_TP

    def mlp_block(row_block):
        hidden = jnp.square(jax.nn.relu(jnp.dot(row_block, up_weight, preferred_element_type=jnp.float32))).astype(jnp.bfloat16)
        total = jnp.zeros((row_block.shape[0], D), jnp.float32)
        for group in range(N_TP):
            partial_sum = jnp.dot(hidden[:, group * hidden_width:(group + 1) * hidden_width], down_weight[group * hidden_width:(group + 1) * hidden_width], preferred_element_type=jnp.float32).astype(jnp.bfloat16)
            total = total + lax.optimization_barrier(partial_sum).astype(jnp.float32)
        mlp_out = lax.optimization_barrier(total.astype(jnp.bfloat16))
        return layer_norm(row_block.astype(jnp.float32) + mlp_out.astype(jnp.float32), out_gain).astype(jnp.bfloat16)
    blocks = first_norm.reshape(SEQUENCE_TOKENS // TOK_DEV, TOK_DEV, D)
    return lax.map(mlp_block, blocks).reshape(SEQUENCE_TOKENS, D)
```

```python
import functools

import jax
import jax.numpy as jnp
from jax import lax
from jax.experimental import pallas as pl
from jax.experimental.pallas import tpu as pltpu
from jax.sharding import PartitionSpec as P

NEG_BIG = -1e30
EPS = 1e-05
F32 = jnp.float32
BF16 = jnp.bfloat16
MESH_ID = pl.DeviceIdType.MESH


def dot(a, b):
    return jnp.dot(a, b, preferred_element_type=F32)


def halves(a):
    high = a.astype(BF16)
    return high, (a - high.astype(F32)).astype(BF16)


def dot_left(a, b):
    high, low = halves(a)
    return dot(high, b) + dot(low, b)


def dot_right(a, b):
    high, low = halves(b)
    return dot(a, high) + dot(a, low)


def layer_norm(rows_f, gain):
    center = jnp.mean(rows_f, -1, keepdims=True)
    spread = jnp.mean(jnp.square(rows_f - center), -1, keepdims=True)
    return (rows_f - center) * lax.rsqrt(spread + EPS) * gain


def kernel(
    ns, ntp, nt, early,
    q1, k1, q2, k2, v, og, ig, fg, hg, ow, stream, mg, up, down, outg,
    out,
    up_slab, dn_slab, ow_v, state, sh_in, sh_out, c_in, small, small_all, peaks, norms,
    mixed, part, mix_in, xg, pbuf, tp_in, rs_out, rs_in,
    own_sem, up_s, up_r, dn_s, dn_r, st_s, st_r, sm_s, sm_r, ci_s, ci_r, mx_s, mx_r,
    ag_s, ag_r, fw_s, tp_s, tp_r, rs_s, rs_r,
):
    s = lax.axis_index("sp")
    c = lax.axis_index("tp")
    nw = ns // nt
    w, t = s // nt, lax.rem(s, nt)
    length = q1.shape[0]
    gates = ig.shape[0]
    pairs = gates // 2
    ka, kb = q1.shape[1] // pairs, q2.shape[1] // pairs
    dv = v.shape[1] // gates
    depth = up.shape[0]
    width = up_slab.shape[1]
    own = out.shape[0]
    shard = sh_in.shape[1]

    def remote(src, dst, send, recv, sp, tp):
        return pltpu.make_async_remote_copy(
            src_ref=src, dst_ref=dst, send_sem=send, recv_sem=recv,
            device_id=(sp, tp), device_id_type=MESH_ID,
        )

    def loop(low, high, fn):
        def step(i, carry):
            fn(i)
            return carry

        lax.fori_loop(low, high, step, 0)

    def peer(j):
        return lax.rem(s + j, ns)

    def mate(j):
        return lax.rem(c + j, ntp)

    barrier = pltpu.get_barrier_semaphore()
    loop(1, ns, lambda j: pl.semaphore_signal(
        barrier, inc=1, device_id=(peer(j), c), device_id_type=MESH_ID))
    loop(1, ntp, lambda j: pl.semaphore_signal(
        barrier, inc=1, device_id=(s, mate(j)), device_id_type=MESH_ID))

    def up_part(which):
        return up.at[:, pl.ds(pl.multiple_of(which * width, 128), width)]

    def dn_part(which):
        return down.at[pl.ds(pl.multiple_of(which * width, 128), width), :]

    def up_rows(source):
        return up_slab.at[pl.ds(pl.multiple_of(source * depth, depth), depth), :]

    own_up = pltpu.make_async_copy(up_part(w), up_rows(s), own_sem.at[0])
    own_dn = pltpu.make_async_copy(dn_part(w), dn_slab.at[s], own_sem.at[1])
    own_ow = pltpu.make_async_copy(ow, ow_v, own_sem.at[2])
    own_ow.start()
    own_up.start()
    own_dn.start()

    def up_copy(j):
        to = peer(j)
        return remote(up_part(to // nt), up_rows(s), up_s.at[j], up_r.at[s], to, c)

    def dn_copy(j):
        to = peer(j)
        return remote(dn_part(to // nt), dn_slab.at[s], dn_s.at[j], dn_r.at[s], to, c)

    pl.semaphore_wait(barrier, ns - 1 + ntp - 1)
    loop(1, early, lambda j: up_copy(j).start())

    forget = fg[...]
    log_forget = jnp.minimum(forget, 0.0) - jnp.log1p(jnp.exp(-jnp.abs(forget)))
    row_id = lax.broadcasted_iota(jnp.int32, (length, length), 0)
    col_id = lax.broadcasted_iota(jnp.int32, (length, length), 1)
    causal = row_id >= col_id
    upper = (row_id <= col_id).astype(F32)
    eye = (row_id == col_id).astype(F32)
    exact = lax.Precision.HIGHEST
    cumulative = jnp.dot(log_forget, upper, precision=exact, preferred_element_type=F32)
    log_input = ig[...]
    total = cumulative[:, length - 1:length]
    weight_log = total - cumulative + log_input
    peak = jnp.max(weight_log, 1, keepdims=True)
    weight = jnp.exp(weight_log - peak)
    key_t1 = jnp.transpose(k1[...].astype(F32))
    key_t2 = jnp.transpose(k2[...].astype(F32))
    norm_1 = dot_left(weight, k1[...]) * ka ** -0.5
    norm_2 = dot_left(weight, k2[...]) * kb ** -0.5
    norm_rows = []
    used = pairs * (ka + kb)
    if used < state.shape[0]:
        state[used:, :] = jnp.zeros((state.shape[0] - used, dv), F32)
    heads = []
    for g in range(gates):
        j, two = g // 2, g % 2
        size = kb if two else ka
        base = pairs * ka * two + j * size
        key_t = (key_t2 if two else key_t1)[j * size:(j + 1) * size]
        query = (q2 if two else q1)[:, j * size:(j + 1) * size]
        heads.append((size, base, key_t, query))
        state[base:base + size, :] = dot_left(
            key_t * (weight[g:g + 1] * size ** -0.5), v[:, g * dv:(g + 1) * dv])
        row = (norm_2 if two else norm_1)[g:g + 1, j * size:(j + 1) * size]
        if size < ka:
            row = jnp.concatenate([row, jnp.zeros((1, ka - size), F32)], 1)
        norm_rows.append(row)
    small[0] = jnp.broadcast_to(total, (gates, ka))
    small[1] = jnp.broadcast_to(peak, (gates, ka))
    small[2] = jnp.concatenate(norm_rows, 0)

    def rows_of(which):
        return pl.ds(pl.multiple_of(which * shard, 8), shard)

    def small_copy(j):
        return remote(small, small_all.at[s], sm_s.at[j], sm_r.at[s], peer(j), c)

    def state_copy(j):
        to = peer(j)
        return remote(state.at[rows_of(to), :], sh_in.at[s], st_s.at[j], st_r.at[s], to, c)

    def first_sends(j):
        small_copy(j).start()
        state_copy(j).start()

    loop(1, ns, first_sends)
    loop(early, ns, lambda j: up_copy(j).start())
    small_all[s] = small[...]
    sh_in[s] = state[rows_of(s), :]

    def first_waits(j):
        source = peer(j)
        remote(small, small_all.at[source], sm_s.at[j], sm_r.at[source], source, c).wait_recv()
        remote(state.at[rows_of(s), :], sh_in.at[source], st_s.at[j], st_r.at[source],
               source, c).wait_recv()

    loop(1, ns, first_waits)

    shard_row = s * shard + lax.broadcasted_iota(jnp.int32, (shard, dv), 0)

    def spread(rows):
        full = jnp.zeros((shard, dv), F32)
        for g in range(gates):
            size, base = heads[g][:2]
            inside = (shard_row >= base) & (shard_row < base + size)
            full = jnp.where(inside, rows[g:g + 1, :], full)
        return full

    def advance(e, carry):
        run, peak_run, norm_run = carry
        sh_out[e] = run
        peaks[e] = peak_run
        norms[e] = norm_run
        decayed = peak_run + small_all[e, 0]
        fresh = small_all[e, 1]
        ceiling = jnp.maximum(decayed, fresh)
        keep = jnp.exp(decayed - ceiling)
        new = jnp.exp(fresh - ceiling)
        return (
            run * spread(keep) + sh_in[e] * spread(new),
            ceiling,
            norm_run * keep + small_all[e, 2] * new,
        )

    lax.fori_loop(0, ns, advance, (
        jnp.zeros((shard, dv), F32),
        jnp.full((gates, ka), NEG_BIG, F32),
        jnp.zeros((gates, ka), F32),
    ))

    def back_copy(j):
        to = peer(j)
        return remote(sh_out.at[to], c_in.at[rows_of(s), :], ci_s.at[j], ci_r.at[s], to, c)

    loop(1, ns, lambda j: back_copy(j).start())
    loop(1, ns, lambda j: dn_copy(j).start())
    c_in[rows_of(s), :] = sh_out[s]
    peak_in = peaks[s]
    norm_in = norms[s]

    cum_cols = lax.dot_general(eye, cumulative, (((1,), (1,)), ((), ())), precision=exact,
                               preferred_element_type=F32)
    column = log_input - cumulative

    def back_waits(j):
        source = peer(j)
        remote(sh_out.at[s], c_in.at[rows_of(source), :], ci_s.at[j], ci_r.at[source],
               source, c).wait_recv()

    inside = []
    for g in range(gates):
        size, base, key_t, query = heads[g]
        cum_col = cum_cols[:, g:g + 1]
        gaps = jnp.where(causal, cum_col + column[g:g + 1], NEG_BIG)
        carried = cum_col + peak_in[g:g + 1, 0:1]
        ceiling = jnp.maximum(carried, jnp.max(gaps, 1, keepdims=True))
        scores = dot(query, key_t.astype(BF16)) * size ** -0.5 * jnp.exp(gaps - ceiling)
        carry_weight = jnp.exp(carried - ceiling)
        numerator = dot_left(scores, v[:, g * dv:(g + 1) * dv])
        denominator = carry_weight * jnp.sum(
            query.astype(F32) * norm_in[g:g + 1, :size], 1, keepdims=True)
        denominator = denominator + jnp.sum(scores, 1, keepdims=True)
        bound = jnp.maximum(jnp.abs(denominator), jnp.exp(-ceiling))
        inside.append((numerator, carry_weight, bound))
    loop(1, ns, back_waits)
    for g in range(gates):
        size, base, key_t, query = heads[g]
        numerator, carry_weight, bound = inside[g]
        cell = (numerator + carry_weight * dot_right(query, c_in[base:base + size, :])) / bound
        center = jnp.mean(cell, -1, keepdims=True)
        variance = jnp.mean(jnp.square(cell - center), -1, keepdims=True)
        cols = slice(g * dv, (g + 1) * dv)
        gate = jax.nn.sigmoid(og[:, cols].astype(F32))
        mixed[:, cols] = (
            (cell - center) * lax.rsqrt(variance + EPS) * hg[:, cols] * gate).astype(BF16)

    own_ow.wait()
    for p in range(0, ow.shape[1], 512):
        part[:, p:p + 512] = dot(mixed[...], ow_v[:, p:p + 512]).astype(BF16)

    def own_block(which):
        return pl.ds(pl.multiple_of(which * own, own), own)

    def mix_copy(j):
        to = mate(j)
        return remote(part.at[own_block(to), :], mix_in.at[c], mx_s.at[j], mx_r.at[c], s, to)

    loop(1, ntp, lambda j: mix_copy(j).start())
    mix_in[c] = part[own_block(c), :]
    for j in range(1, ntp):
        source = mate(j)
        remote(part.at[own_block(c), :], mix_in.at[source], mx_s.at[j], mx_r.at[source],
               s, source).wait_recv()
    mixer = mix_in[0].astype(F32)
    for j in range(1, ntp):
        mixer = mixer + mix_in[j].astype(F32)
    mixer = mixer.astype(BF16).astype(F32)
    first = layer_norm(stream[own_block(c), :].astype(F32) + mixer, mg[...]).astype(BF16)
    xg[w * ntp + c] = first

    def group(j):
        return lax.rem(w + j, nw)

    def share_copy(j):
        slot = w * ntp + c
        return remote(xg.at[slot], xg.at[slot], ag_s.at[j], ag_r.at[slot], group(j) * nt + t, c)

    def hand_copy(from_w, j):
        slot = from_w * ntp + c
        return remote(xg.at[slot], xg.at[slot], fw_s.at[from_w * ntp + j], ag_r.at[slot],
                      s, mate(j))

    loop(1, nw, lambda j: share_copy(j).start())
    loop(1, ntp, lambda j: hand_copy(w, j).start())

    def slot_wait(slot):
        remote(xg.at[slot], xg.at[slot], ag_s.at[0], ag_r.at[slot], s, c).wait_recv()

    own_up.wait()
    own_dn.wait()

    def weight_waits(j):
        source = peer(j)
        remote(up_part(w), up_rows(source), up_s.at[j], up_r.at[source], source, c).wait_recv()
        remote(dn_part(w), dn_slab.at[source], dn_s.at[j], dn_r.at[source], source, c).wait_recv()

    joined = max(1, 256 // depth)

    def arrive(j):
        from_w = group(nw - j)
        slot_wait(from_w * ntp + c)
        loop(1, ntp, lambda i: hand_copy(from_w, i).start())

    def tp_copy(to_w, j):
        to = mate(j)
        return remote(pbuf.at[to_w, own_block(to), :], tp_in.at[to_w, c],
                      tp_s.at[to_w * ntp + j], tp_r.at[to_w * ntp + c], s, to)

    def mixer_step(j):
        from_w = group(nw - j)
        loop(1, ntp, lambda i: slot_wait(from_w * ntp + mate(i)))
        rows = xg[pl.ds(from_w * ntp, ntp)].reshape(ntp * own, xg.shape[2])
        hidden = jnp.square(jnp.maximum(dot(rows, up_slab[...]), 0.0)).astype(BF16)
        for a in range(0, ns, joined):
            block = jnp.concatenate([dn_slab[a + i] for i in range(joined)], 1)
            pbuf[from_w, :, a * depth:(a + joined) * depth] = dot(hidden, block).astype(BF16)
        loop(1, ntp, lambda i: tp_copy(from_w, i).start())

    def sum_copy(to_w, j):
        return remote(rs_out.at[to_w], rs_in.at[w], rs_s.at[j], rs_r.at[w], to_w * nt + t, c)

    def pair_sum(j):
        to_w = group(nw - j)
        for i in range(1, ntp):
            source = mate(i)
            remote(pbuf.at[to_w, own_block(c), :], tp_in.at[to_w, source],
                   tp_s.at[to_w * ntp + i], tp_r.at[to_w * ntp + source], s, source).wait_recv()
        added = pbuf[to_w, own_block(c), :].astype(F32)
        for i in range(1, ntp):
            added = added + tp_in[to_w, mate(i)].astype(F32)
        return to_w, added.astype(BF16)

    def send_sum(j):
        to_w, added = pair_sum(j)
        rs_out[to_w] = added
        sum_copy(to_w, j).start()

    loop(1, ns, weight_waits)
    arrive(1)

    def step(j, carry):
        @pl.when(j < nw - 1)
        def _():
            arrive(j + 1)

        mixer_step(j)

        @pl.when(j > 1)
        def _():
            send_sum(j - 1)

        return carry

    lax.fori_loop(1, nw, step, 0)
    mixer_step(nw)
    send_sum(nw - 1)
    _, added = pair_sum(nw)
    rs_in[w] = added

    def sum_wait(j):
        source = group(j)
        remote(rs_out.at[source], rs_in.at[source], rs_s.at[j], rs_r.at[source],
               source * nt + t, c).wait_recv()

    loop(1, nw, sum_wait)
    mlp_out = rs_in[0].astype(F32)
    for i in range(1, nw):
        mlp_out = mlp_out + rs_in[i].astype(F32)
    mlp_out = mlp_out.astype(BF16).astype(F32)
    out[...] = layer_norm(xg[w * ntp + c].astype(F32) + mlp_out, outg[...]).astype(BF16)

    def drain(j):
        up_copy(j).wait_send()
        dn_copy(j).wait_send()
        small_copy(j).wait_send()
        state_copy(j).wait_send()
        back_copy(j).wait_send()

    loop(1, ns, drain)
    loop(1, ntp, lambda j: mix_copy(j).wait_send())

    def drain_group(j):
        share_copy(j).wait_send()
        sum_copy(group(nw - j), j).wait_send()

    loop(1, nw, drain_group)

    def drain_pair(a):
        for j in range(1, ntp):
            hand_copy(a, j).wait_send()
            tp_copy(a, j).wait_send()

    loop(0, nw, drain_pair)


def body(mesh, *args):
    (q1, k1, q2, k2, v, og, ig, fg, hg, ow, stream, mg, up, down, outg) = args
    ns, ntp = mesh.shape["sp"], mesh.shape["tp"]
    nt = 2
    while (up.shape[1] // (ns // nt)) % 128:
        nt *= 2
    nw = ns // nt
    width = up.shape[1] // nw
    depth = up.shape[0]
    length, model = stream.shape
    own = length // ntp
    gates = ig.shape[0]
    dv = v.shape[1] // gates
    ka = 2 * q1.shape[1] // gates
    used = q1.shape[1] + q2.shape[1]
    shard = -(-used // (ns * 8)) * 8
    vm = pl.BlockSpec(memory_space=pltpu.VMEM)
    hbm = pl.BlockSpec(memory_space=pl.ANY)
    sem = pltpu.SemaphoreType.DMA
    return pl.pallas_call(
        functools.partial(kernel, ns, ntp, nt, ns // 2),
        out_shape=jax.ShapeDtypeStruct((own, model), BF16),
        in_specs=[vm] * 9 + [hbm, vm, vm, hbm, hbm, vm],
        out_specs=vm,
        scratch_shapes=[
            pltpu.VMEM((model, width), BF16),
            pltpu.VMEM((ns, width, depth), BF16),
            pltpu.VMEM(ow.shape, BF16),
            pltpu.VMEM((ns * shard, dv), F32),
            pltpu.VMEM((ns, shard, dv), F32),
            pltpu.VMEM((ns, shard, dv), F32),
            pltpu.VMEM((ns * shard, dv), F32),
            pltpu.VMEM((3, gates, ka), F32),
            pltpu.VMEM((ns, 3, gates, ka), F32),
            pltpu.VMEM((ns, gates, ka), F32),
            pltpu.VMEM((ns, gates, ka), F32),
            pltpu.VMEM((length, v.shape[1]), BF16),
            pltpu.VMEM((length, model), BF16),
            pltpu.VMEM((ntp, own, model), BF16),
            pltpu.VMEM((nw * ntp, own, model), BF16),
            pltpu.VMEM((nw, length, model), BF16),
            pltpu.VMEM((nw, ntp, own, model), BF16),
            pltpu.VMEM((nw, own, model), BF16),
            pltpu.VMEM((nw, own, model), BF16),
            sem((3,)),
        ] + [sem((ns,))] * 10 + [sem((ntp,))] * 2 + [
            sem((nw,)), sem((nw * ntp,)), sem((nw * ntp,)), sem((nw * ntp,)),
            sem((nw * ntp,)), sem((nw,)), sem((nw,)),
        ],
        compiler_params=pltpu.CompilerParams(
            collective_id=0, has_side_effects=True, vmem_limit_bytes=60 * 1024 * 1024),
    )(q1, k1, q2, k2, v, og, ig, fg, hg.reshape(1, -1), ow, stream, mg.reshape(1, -1),
      up, down, outg.reshape(1, -1))


def solution(mesh):
    in_specs = (
        P("sp", "tp"),
        P("sp", "tp"),
        P("sp", "tp"),
        P("sp", "tp"),
        P("sp", "tp"),
        P("sp", "tp"),
        P("tp", "sp"),
        P("tp", "sp"),
        P("tp"),
        P("tp", None),
        P("sp", None),
        P(),
        P("sp", "tp"),
        P("tp", "sp"),
        P(),
    )
    out_specs = P(("sp", "tp"), None)
    return jax.shard_map(functools.partial(body, mesh), mesh=mesh, in_specs=in_specs,
                         out_specs=out_specs, check_vma=False)
```

```python
import functools

import jax
import jax.numpy as jnp
from jax import lax
from jax.experimental import pallas as pl
from jax.experimental.pallas import tpu as pltpu
from jax.sharding import PartitionSpec as P

NEG_BIG = -1e30
EPS = 1e-05
F32 = jnp.float32
BF16 = jnp.bfloat16
MESH_ID = pl.DeviceIdType.MESH


def dot(a, b):
    return jnp.dot(a, b, preferred_element_type=F32)


def halves(a):
    high = a.astype(BF16)
    return high, (a - high.astype(F32)).astype(BF16)


def dot_left(a, b):
    high, low = halves(a)
    return dot(high, b) + dot(low, b)


def dot_right(a, b):
    high, low = halves(b)
    return dot(a, high) + dot(a, low)


def layer_norm(rows_f, gain):
    center = jnp.mean(rows_f, -1, keepdims=True)
    spread = jnp.mean(jnp.square(rows_f - center), -1, keepdims=True)
    return (rows_f - center) * lax.rsqrt(spread + EPS) * gain


def kernel(
    ns, ntp, nt, ny,
    q1, k1, q2, k2, v, og, ig, fg, hg, ow, stream, mg, up, down, outg,
    out,
    up_slab, dn_slab, ow_v, state, sh_in, sh_out, c_in, small, small_all, peaks, norms,
    mixed, part, mix_in, xg, pbuf, tp_in, y_out, y_in, rs_out, rs_in,
    own_sem, up_f, dn_f, up_s, up_r, dn_s, dn_r, st_s, st_r, sm_s, sm_r, ci_s, ci_r, mx_s, mx_r,
    ag_s, yf_s, yr_s, yr_r, ag_r, fw_s, tp_s, tp_r, rs_s, rs_r,
):
    s = lax.axis_index("sp")
    c = lax.axis_index("tp")
    nw = ns // nt
    w, t = s // nt, lax.rem(s, nt)
    nz = nw // ny
    z, y = w // ny, lax.rem(w, ny)
    length = q1.shape[0]
    gates = ig.shape[0]
    pairs = gates // 2
    ka, kb = q1.shape[1] // pairs, q2.shape[1] // pairs
    dv = v.shape[1] // gates
    depth = up.shape[0]
    width = up_slab.shape[1]
    own = out.shape[0]
    shard = sh_in.shape[1]

    def remote(src, dst, send, recv, sp, tp):
        return pltpu.make_async_remote_copy(
            src_ref=src, dst_ref=dst, send_sem=send, recv_sem=recv,
            device_id=(sp, tp), device_id_type=MESH_ID,
        )

    def loop(low, high, fn):
        def step(i, carry):
            fn(i)
            return carry

        lax.fori_loop(low, high, step, 0)

    def peer(j):
        return lax.rem(s + j, ns)

    def mate(j):
        return lax.rem(c + j, ntp)

    barrier = pltpu.get_barrier_semaphore()
    loop(1, ns, lambda j: pl.semaphore_signal(
        barrier, inc=1, device_id=(peer(j), c), device_id_type=MESH_ID))
    loop(1, ntp, lambda j: pl.semaphore_signal(
        barrier, inc=1, device_id=(s, mate(j)), device_id_type=MESH_ID))

    def up_part(which):
        return up.at[:, pl.ds(pl.multiple_of(which * width, 128), width)]

    def dn_part(which):
        return down.at[pl.ds(pl.multiple_of(which * width, 128), width), :]

    def up_rows(source):
        return up_slab.at[pl.ds(pl.multiple_of(source * depth, depth), depth), :]

    own_up = pltpu.make_async_copy(up_part(w), up_rows(s), own_sem.at[0])
    own_dn = pltpu.make_async_copy(dn_part(w), dn_slab.at[s], own_sem.at[1])
    own_ow = pltpu.make_async_copy(ow, ow_v, own_sem.at[2])
    own_ow.start()
    own_up.start()
    own_dn.start()

    def up_copy(j):
        to = lax.rem(w + j, nw)
        return remote(up_part(to), up_rows(s), up_s.at[j], up_r.at[s], to * nt + t, c)

    def dn_copy(j):
        to = lax.rem(w + j, nw)
        return remote(dn_part(to), dn_slab.at[s], dn_s.at[j], dn_r.at[s], to * nt + t, c)

    def up_hand(j, i):
        source = lax.rem(w + nw - j, nw) * nt + t
        return remote(up_rows(source), up_rows(source), up_f.at[j * nt + i],
                      up_r.at[source], w * nt + lax.rem(t + i, nt), c)

    def dn_hand(j, i):
        source = lax.rem(w + nw - j, nw) * nt + t
        return remote(dn_slab.at[source], dn_slab.at[source], dn_f.at[j * nt + i],
                      dn_r.at[source], w * nt + lax.rem(t + i, nt), c)

    def up_wait(source):
        remote(up_part(w), up_rows(source), up_s.at[0], up_r.at[source], peer(1), c).wait_recv()

    def dn_wait(source):
        remote(dn_part(w), dn_slab.at[source], dn_s.at[0], dn_r.at[source], peer(1),
               c).wait_recv()

    def up_pass(j):
        up_wait(lax.rem(w + nw - j, nw) * nt + t)
        loop(1, nt, lambda i: up_hand(j, i).start())

    def dn_pass(j):
        dn_wait(lax.rem(w + nw - j, nw) * nt + t)
        loop(1, nt, lambda i: dn_hand(j, i).start())

    pl.semaphore_wait(barrier, ns - 1 + ntp - 1)
    loop(1, nw // 2, lambda j: up_copy(j).start())

    forget = fg[...]
    log_forget = jnp.minimum(forget, 0.0) - jnp.log1p(jnp.exp(-jnp.abs(forget)))
    row_id = lax.broadcasted_iota(jnp.int32, (length, length), 0)
    col_id = lax.broadcasted_iota(jnp.int32, (length, length), 1)
    causal = row_id >= col_id
    upper = (row_id <= col_id).astype(F32)
    eye = (row_id == col_id).astype(F32)
    exact = lax.Precision.HIGHEST
    cumulative = jnp.dot(log_forget, upper, precision=exact, preferred_element_type=F32)
    log_input = ig[...]
    total = cumulative[:, length - 1:length]
    weight_log = total - cumulative + log_input
    peak = jnp.max(weight_log, 1, keepdims=True)
    weight = jnp.exp(weight_log - peak)
    key_t1 = jnp.transpose(k1[...].astype(F32))
    key_t2 = jnp.transpose(k2[...].astype(F32))
    norm_1 = dot_left(weight, k1[...]) * ka ** -0.5
    norm_2 = dot_left(weight, k2[...]) * kb ** -0.5
    norm_rows = []
    used = pairs * (ka + kb)
    if used < state.shape[0]:
        state[used:, :] = jnp.zeros((state.shape[0] - used, dv), F32)
    heads = []
    for g in range(gates):
        j, two = g // 2, g % 2
        size = kb if two else ka
        base = pairs * ka * two + j * size
        key_t = (key_t2 if two else key_t1)[j * size:(j + 1) * size]
        query = (q2 if two else q1)[:, j * size:(j + 1) * size]
        heads.append((size, base, key_t, query))
        state[base:base + size, :] = dot_left(
            key_t * (weight[g:g + 1] * size ** -0.5), v[:, g * dv:(g + 1) * dv])
        row = (norm_2 if two else norm_1)[g:g + 1, j * size:(j + 1) * size]
        if size < ka:
            row = jnp.concatenate([row, jnp.zeros((1, ka - size), F32)], 1)
        norm_rows.append(row)
    small[0] = jnp.broadcast_to(total, (gates, ka))
    small[1] = jnp.broadcast_to(peak, (gates, ka))
    small[2] = jnp.concatenate(norm_rows, 0)

    def rows_of(which):
        return pl.ds(pl.multiple_of(which * shard, 8), shard)

    def small_copy(j):
        return remote(small, small_all.at[s], sm_s.at[j], sm_r.at[s], peer(j), c)

    def state_copy(j):
        to = peer(j)
        return remote(state.at[rows_of(to), :], sh_in.at[s], st_s.at[j], st_r.at[s], to, c)

    def first_sends(j):
        small_copy(j).start()
        state_copy(j).start()

    loop(1, ns, first_sends)
    loop(nw // 2, nw, lambda j: up_copy(j).start())
    small_all[s] = small[...]
    sh_in[s] = state[rows_of(s), :]

    def first_waits(j):
        source = peer(j)
        remote(small, small_all.at[source], sm_s.at[j], sm_r.at[source], source, c).wait_recv()
        remote(state.at[rows_of(s), :], sh_in.at[source], st_s.at[j], st_r.at[source],
               source, c).wait_recv()

    loop(1, ns, first_waits)

    shard_row = s * shard + lax.broadcasted_iota(jnp.int32, (shard, dv), 0)

    def spread(rows):
        full = jnp.zeros((shard, dv), F32)
        for g in range(gates):
            size, base = heads[g][:2]
            inside = (shard_row >= base) & (shard_row < base + size)
            full = jnp.where(inside, rows[g:g + 1, :], full)
        return full

    def advance(e, carry):
        run, peak_run, norm_run = carry
        sh_out[e] = run
        peaks[e] = peak_run
        norms[e] = norm_run
        decayed = peak_run + small_all[e, 0]
        fresh = small_all[e, 1]
        ceiling = jnp.maximum(decayed, fresh)
        keep = jnp.exp(decayed - ceiling)
        new = jnp.exp(fresh - ceiling)
        return (
            run * spread(keep) + sh_in[e] * spread(new),
            ceiling,
            norm_run * keep + small_all[e, 2] * new,
        )

    lax.fori_loop(0, ns, advance, (
        jnp.zeros((shard, dv), F32),
        jnp.full((gates, ka), NEG_BIG, F32),
        jnp.zeros((gates, ka), F32),
    ))

    def back_copy(j):
        to = peer(j)
        return remote(sh_out.at[to], c_in.at[rows_of(s), :], ci_s.at[j], ci_r.at[s], to, c)

    loop(1, ns, lambda j: back_copy(j).start())
    loop(1, nw, lambda j: dn_copy(j).start())
    own_up.wait()
    loop(1, nt, lambda i: up_hand(0, i).start())
    loop(1, nw, up_pass)
    c_in[rows_of(s), :] = sh_out[s]
    peak_in = peaks[s]
    norm_in = norms[s]

    cum_cols = lax.dot_general(eye, cumulative, (((1,), (1,)), ((), ())), precision=exact,
                               preferred_element_type=F32)
    column = log_input - cumulative

    def back_waits(j):
        source = peer(j)
        remote(sh_out.at[s], c_in.at[rows_of(source), :], ci_s.at[j], ci_r.at[source],
               source, c).wait_recv()

    inside = []
    for g in range(gates):
        size, base, key_t, query = heads[g]
        cum_col = cum_cols[:, g:g + 1]
        gaps = jnp.where(causal, cum_col + column[g:g + 1], NEG_BIG)
        carried = cum_col + peak_in[g:g + 1, 0:1]
        ceiling = jnp.maximum(carried, jnp.max(gaps, 1, keepdims=True))
        scores = dot(query, key_t.astype(BF16)) * size ** -0.5 * jnp.exp(gaps - ceiling)
        carry_weight = jnp.exp(carried - ceiling)
        numerator = dot_left(scores, v[:, g * dv:(g + 1) * dv])
        denominator = carry_weight * jnp.sum(
            query.astype(F32) * norm_in[g:g + 1, :size], 1, keepdims=True)
        denominator = denominator + jnp.sum(scores, 1, keepdims=True)
        bound = jnp.maximum(jnp.abs(denominator), jnp.exp(-ceiling))
        inside.append((numerator, carry_weight, bound))
    loop(1, ns, back_waits)
    for g in range(gates):
        size, base, key_t, query = heads[g]
        numerator, carry_weight, bound = inside[g]
        cell = (numerator + carry_weight * dot_right(query, c_in[base:base + size, :])) / bound
        center = jnp.mean(cell, -1, keepdims=True)
        variance = jnp.mean(jnp.square(cell - center), -1, keepdims=True)
        cols = slice(g * dv, (g + 1) * dv)
        gate = jax.nn.sigmoid(og[:, cols].astype(F32))
        mixed[:, cols] = (
            (cell - center) * lax.rsqrt(variance + EPS) * hg[:, cols] * gate).astype(BF16)

    own_ow.wait()
    for p in range(0, ow.shape[1], 512):
        part[:, p:p + 512] = dot(mixed[...], ow_v[:, p:p + 512]).astype(BF16)

    def own_block(which):
        return pl.ds(pl.multiple_of(which * own, own), own)

    def mix_copy(j):
        to = mate(j)
        return remote(part.at[own_block(to), :], mix_in.at[c], mx_s.at[j], mx_r.at[c], s, to)

    loop(1, ntp, lambda j: mix_copy(j).start())
    mix_in[c] = part[own_block(c), :]
    for j in range(1, ntp):
        source = mate(j)
        remote(part.at[own_block(c), :], mix_in.at[source], mx_s.at[j], mx_r.at[source],
               s, source).wait_recv()
    mixer = mix_in[0].astype(F32)
    for j in range(1, ntp):
        mixer = mixer + mix_in[j].astype(F32)
    mixer = mixer.astype(BF16).astype(F32)
    first = layer_norm(stream[own_block(c), :].astype(F32) + mixer, mg[...]).astype(BF16)
    xg[w * ntp + c] = first

    def hand_copy(from_w, j):
        slot = from_w * ntp + c
        return remote(xg.at[slot], xg.at[slot], fw_s.at[from_w * ntp + j], ag_r.at[slot],
                      s, mate(j))

    def sp_of(to_z, to_y):
        return (to_z * ny + to_y) * nt + t

    def z_of(j):
        return lax.rem(z + j, nz)

    def y_of(j):
        return lax.rem(y + j, ny)

    def share_copy(j):
        slot = w * ntp + c
        return remote(xg.at[slot], xg.at[slot], ag_s.at[j], ag_r.at[slot], sp_of(z_of(j), y), c)

    def over_y(from_z, j):
        slot = (from_z * ny + y) * ntp + c
        return remote(xg.at[slot], xg.at[slot], yf_s.at[from_z * ny + j], ag_r.at[slot],
                      sp_of(z, y_of(j)), c)

    def slot_wait(slot):
        remote(xg.at[slot], xg.at[slot], ag_s.at[0], ag_r.at[slot], peer(1), c).wait_recv()

    def pass_on(from_z):
        loop(1, ny, lambda i: over_y(from_z, i).start())
        loop(1, ntp, lambda i: hand_copy(from_z * ny + y, i).start())

    def arrive(j):
        from_z = z_of(nz - j)
        slot_wait((from_z * ny + y) * ntp + c)
        pass_on(from_z)

    loop(1, nz, lambda j: share_copy(j).start())
    pass_on(z)

    own_dn.wait()
    loop(1, nt, lambda i: dn_hand(0, i).start())
    loop(1, nw, dn_pass)

    def other_waits(j):
        source = (j // (nt - 1)) * nt + lax.rem(t + 1 + lax.rem(j, nt - 1), nt)
        up_wait(source)
        dn_wait(source)

    joined = max(1, 256 // depth)

    def tp_copy(to_w, j):
        to = mate(j)
        return remote(pbuf.at[to_w, own_block(to), :], tp_in.at[to_w, c],
                      tp_s.at[to_w * ntp + j], tp_r.at[to_w * ntp + c], s, to)

    def mixer_step(from_w):
        loop(1, ntp, lambda i: slot_wait(from_w * ntp + mate(i)))
        rows = xg[pl.ds(from_w * ntp, ntp)].reshape(ntp * own, xg.shape[2])
        hidden = jnp.square(jnp.maximum(dot(rows, up_slab[...]), 0.0)).astype(BF16)
        for a in range(0, ns, joined):
            block = jnp.concatenate([dn_slab[a + i] for i in range(joined)], 1)
            pbuf[from_w, :, a * depth:(a + joined) * depth] = dot(hidden, block).astype(BF16)
        loop(1, ntp, lambda i: tp_copy(from_w, i).start())

    def pair_sum(to_w):
        for i in range(1, ntp):
            source = mate(i)
            remote(pbuf.at[to_w, own_block(c), :], tp_in.at[to_w, source],
                   tp_s.at[to_w * ntp + i], tp_r.at[to_w * ntp + source], s, source).wait_recv()
        added = pbuf[to_w, own_block(c), :].astype(F32)
        for i in range(1, ntp):
            added = added + tp_in[to_w, mate(i)].astype(F32)
        return added

    def y_copy(to_z, j):
        to = y_of(j)
        return remote(y_out.at[to_z * ny + to], y_in.at[to_z * ny + y],
                      yr_s.at[to_z * ny + j], yr_r.at[to_z * ny + y], sp_of(z, to), c)

    def sum_copy(to_z, j):
        return remote(rs_out.at[to_z], rs_in.at[z], rs_s.at[j], rs_r.at[z], sp_of(to_z, y), c)

    def compute(j):
        at = z_of(nz - j)

        def other(i):
            slot = (at * ny + y_of(i)) * ntp + c
            slot_wait(slot)
            loop(1, ntp, lambda k: hand_copy(at * ny + y_of(i), k).start())

        loop(1, ny, other)
        mixer_step(at * ny + y)

        def other_step(i):
            to = at * ny + y_of(i)
            mixer_step(to)
            y_out[to] = pair_sum(to).astype(BF16)
            y_copy(at, i).start()

        loop(1, ny, other_step)

    def collect(j):
        at = z_of(nz - j)
        added = pair_sum(at * ny + y)
        for i in range(1, ny):
            source = at * ny + y_of(i)
            remote(y_out.at[source], y_in.at[source], yr_s.at[0], yr_r.at[source],
                   peer(1), c).wait_recv()
            added = added + y_in[source].astype(F32)
        return at, added.astype(BF16)

    def send_sum(j):
        to_z, added = collect(j)
        rs_out[to_z] = added
        sum_copy(to_z, j).start()

    if nz > 1:
        arrive(1)
    loop(0, nw * (nt - 1), other_waits)

    def step(j, carry):
        @pl.when(j < nz - 1)
        def _():
            arrive(j + 1)

        compute(j)

        @pl.when(j > 1)
        def _():
            send_sum(j - 1)

        return carry

    lax.fori_loop(1, nz, step, 0)
    compute(nz)
    if nz > 1:
        send_sum(nz - 1)
    _, added = collect(nz)
    rs_in[z] = added

    def sum_wait(j):
        source = z_of(j)
        remote(rs_out.at[source], rs_in.at[source], rs_s.at[j], rs_r.at[source],
               peer(1), c).wait_recv()

    loop(1, nz, sum_wait)
    mlp_out = rs_in[0].astype(F32)
    for i in range(1, nz):
        mlp_out = mlp_out + rs_in[i].astype(F32)
    mlp_out = mlp_out.astype(BF16).astype(F32)
    out[...] = layer_norm(xg[w * ntp + c].astype(F32) + mlp_out, outg[...]).astype(BF16)

    def drain(j):
        small_copy(j).wait_send()
        state_copy(j).wait_send()
        back_copy(j).wait_send()

    loop(1, ns, drain)
    loop(1, ntp, lambda j: mix_copy(j).wait_send())

    def drain_weights(j):
        up_copy(j).wait_send()
        dn_copy(j).wait_send()

    loop(1, nw, drain_weights)

    def drain_hand(j):
        for i in range(1, nt):
            up_hand(j, i).wait_send()
            dn_hand(j, i).wait_send()

    loop(0, nw, drain_hand)

    def drain_group(j):
        share_copy(j).wait_send()
        sum_copy(z_of(nz - j), j).wait_send()

    loop(1, nz, drain_group)

    def drain_y(a):
        for j in range(1, ny):
            over_y(a, j).wait_send()
            y_copy(a, j).wait_send()

    loop(0, nz, drain_y)

    def drain_pair(a):
        for j in range(1, ntp):
            hand_copy(a, j).wait_send()
            tp_copy(a, j).wait_send()

    loop(0, nw, drain_pair)


def body(mesh, *args):
    (q1, k1, q2, k2, v, og, ig, fg, hg, ow, stream, mg, up, down, outg) = args
    ns, ntp = mesh.shape["sp"], mesh.shape["tp"]
    nt = 2
    while (up.shape[1] // (ns // nt)) % 128:
        nt *= 2
    nw = ns // nt
    ny = 2 if nw % 2 == 0 else 1
    width = up.shape[1] // nw
    depth = up.shape[0]
    length, model = stream.shape
    own = length // ntp
    gates = ig.shape[0]
    dv = v.shape[1] // gates
    ka = 2 * q1.shape[1] // gates
    used = q1.shape[1] + q2.shape[1]
    shard = -(-used // (ns * 8)) * 8
    vm = pl.BlockSpec(memory_space=pltpu.VMEM)
    hbm = pl.BlockSpec(memory_space=pl.ANY)
    sem = pltpu.SemaphoreType.DMA
    return pl.pallas_call(
        functools.partial(kernel, ns, ntp, nt, ny),
        out_shape=jax.ShapeDtypeStruct((own, model), BF16),
        in_specs=[vm] * 9 + [hbm, vm, vm, hbm, hbm, vm],
        out_specs=vm,
        scratch_shapes=[
            pltpu.VMEM((model, width), BF16),
            pltpu.VMEM((ns, width, depth), BF16),
            pltpu.VMEM(ow.shape, BF16),
            pltpu.VMEM((ns * shard, dv), F32),
            pltpu.VMEM((ns, shard, dv), F32),
            pltpu.VMEM((ns, shard, dv), F32),
            pltpu.VMEM((ns * shard, dv), F32),
            pltpu.VMEM((3, gates, ka), F32),
            pltpu.VMEM((ns, 3, gates, ka), F32),
            pltpu.VMEM((ns, gates, ka), F32),
            pltpu.VMEM((ns, gates, ka), F32),
            pltpu.VMEM((length, v.shape[1]), BF16),
            pltpu.VMEM((length, model), BF16),
            pltpu.VMEM((ntp, own, model), BF16),
            pltpu.VMEM((nw * ntp, own, model), BF16),
            pltpu.VMEM((nw, length, model), BF16),
            pltpu.VMEM((nw, ntp, own, model), BF16),
            pltpu.VMEM((nw, own, model), BF16),
            pltpu.VMEM((nw, own, model), BF16),
            pltpu.VMEM((nw // ny, own, model), BF16),
            pltpu.VMEM((nw // ny, own, model), BF16),
            sem((3,)),
        ] + [sem((ns,))] * 12 + [sem((ntp,))] * 2 + [
            sem((nw,)), sem((nw,)), sem((nw,)), sem((nw,)), sem((nw * ntp,)), sem((nw * ntp,)), sem((nw * ntp,)),
            sem((nw * ntp,)), sem((nw,)), sem((nw,)),
        ],
        compiler_params=pltpu.CompilerParams(
            collective_id=0, has_side_effects=True, vmem_limit_bytes=60 * 1024 * 1024),
    )(q1, k1, q2, k2, v, og, ig, fg, hg.reshape(1, -1), ow, stream, mg.reshape(1, -1),
      up, down, outg.reshape(1, -1))


def solution(mesh):
    in_specs = (
        P("sp", "tp"),
        P("sp", "tp"),
        P("sp", "tp"),
        P("sp", "tp"),
        P("sp", "tp"),
        P("sp", "tp"),
        P("tp", "sp"),
        P("tp", "sp"),
        P("tp"),
        P("tp", None),
        P("sp", None),
        P(),
        P("sp", "tp"),
        P("tp", "sp"),
        P(),
    )
    out_specs = P(("sp", "tp"), None)
    return jax.shard_map(functools.partial(body, mesh), mesh=mesh, in_specs=in_specs,
                         out_specs=out_specs, check_vma=False)
```
